32 devices in a mesh: ep: 16 (over z, y, x), tp: 2 (over core).
Axes of the slice: x: 2, y: 2, z: 4, core: 2. Of those that a mesh axis runs over, the one named last changes fastest.
Arguments:
- tokens: bfloat16 [256, 2048], P('ep'), may hold values from -6 to 6
- norm_attn: float32 [2048], replicated, may hold values from 0.1 to 1.9
- w_query: bfloat16 [2048, 2048], P(None, 'tp'), may hold values from -0.125 to 0.125
- w_key: bfloat16 [2048, 256], P(None, 'tp'), may hold values from -0.125 to 0.125
- w_value: bfloat16 [2048, 256], P(None, 'tp'), may hold values from -0.125 to 0.125
- w_out: bfloat16 [2048, 2048], P('tp'), may hold values from -0.125 to 0.125
- attn_bias: float32 [32], P('tp'), may hold values from -7 to -1
- cache_keys: bfloat16 [256, 1024, 256], P('ep', None, 'tp'), may hold values from -6 to 6
- cache_values: bfloat16 [256, 1024, 256], P('ep', None, 'tp'), may hold values from -6 to 6
- lengths: int32 [256], P('ep'), may hold values from 256 to 1024
- norm_ffn: float32 [2048], replicated, may hold values from 0.1 to 1.9
- expert_gate: bfloat16 [2048, 57344], P(None, ('ep', 'tp')), may hold values from -0.125 to 0.125
- expert_up: bfloat16 [2048, 57344], P(None, ('ep', 'tp')), may hold values from -0.125 to 0.125
- expert_down: bfloat16 [57344, 2048], P(('ep', 'tp')), may hold values from -0.0625 to 0.0625
- dense_gate_w: bfloat16 [2048, 7168], P(None, 'ep'), may hold values from -0.125 to 0.125
- dense_up_w: bfloat16 [2048, 7168], P(None, 'ep'), may hold values from -0.125 to 0.125
- dense_down_w: bfloat16 [7168, 2048], P('ep'), may hold values from -0.0625 to 0.0625
- dense_mix: bfloat16 [2048], replicated, may hold values from -0.125 to 0.125
- routes: int32 [256, 2], P(('ep', 'tp')), may hold values from 0 to 7, all different within a row; in each aligned block of 8 rows (0 to 7, 8 to 15, ...) at most 3 rows name the same one
- route_weights: bfloat16 [256, 2], P(('ep', 'tp')), may hold values from 0.19921875 to 1
Outputs:
- layer_out: bfloat16 [256, 2048], P(('ep', 'tp'))
- new_keys: bfloat16 [256, 256], P('ep', 'tp')
- new_values: bfloat16 [256, 256], P('ep', 'tp')
The draws below stay inside these ranges and needn't reach their ends.
Inputs may be any that keep to these rules, and one draw needn't show every extreme that they name: `routes`: in each aligned block of 8 rows (the rows of one device) no expert is named by more than 3 rows, a bound that some block reaches; a row names 2 different experts.
All inputs are finite; a program needn't handle non-finite values.
Results may differ from the reference program's by a relative error of at most 0.015.
Values may be sent and summed in bfloat16 or wider, within the bound.
A program may use at most 128 MiB of HBM per device.

```python
import math
import jax
import jax.numpy as jnp
import numpy as np
from jax import lax

D = 2048
HEADS = 32
KV_HEADS = 4
HEAD_DIM = 64
FF = 7168
DENSE_FF = 7168
EXPERTS = 8
TOP = 2
SEQS_DEV = 16
CACHE = 1024
TOKENS = 256
ROWS_DEV = 8
CAP_DEV = 3
N_EP = 16
N_TP = 2


def place_ends(drawn, key, low, largest):
    dims = drawn.shape
    spot = [jax.random.randint(jax.random.fold_in(key, axis), (), 0, dims[axis]) for axis in range(len(dims))]
    drawn = drawn.at[tuple(spot)].set(low)
    longest = dims.index(max(dims))
    spot[longest] = (spot[longest] + 1) % dims[longest]
    return drawn.at[tuple(spot)].set(largest)


def steps_of(own_key, dims, pieces, smallest, top_value):
    def one(position, blocks):
        steps = jax.random.uniform(jax.random.fold_in(jax.random.fold_in(own_key, 6), position), (blocks,), jnp.float32, smallest / len(pieces), top_value / len(pieces))
        return jnp.repeat(jnp.exp(steps), dims[position] // blocks).reshape((-1,) + (1,) * (len(dims) - position - 1))

    level = one(*pieces[0])
    for cut in pieces[1:]:
        level = level * one(*cut)
    return level


def assign_block(key, own, number, rows, count, top, limit, lean):
    sequence = jax.random.permutation(key, count)
    crowded, ordinary = portions_of(count, rows * top, limit, lean, True), portions_of(count, rows * top, limit, lean, False)
    places = jnp.arange(count)

    def named(tallies, rotation):
        used = int((tallies > 0).sum())
        fixed = max(1, used // 4)
        moved = fixed + (places - fixed + rotation * (used - fixed)) % max(1, count - fixed)
        return jnp.zeros((count,), jnp.int32).at[sequence[jnp.where(places < fixed, places, moved)]].set(jnp.asarray(tallies, jnp.int32))

    tallies = jnp.where(number % 4 == 0, named(crowded, number // 4), named(ordinary, number - number // 4 - 1))
    mixed = jax.random.permutation(jax.random.fold_in(own, 3), count)
    source_of, sink = mixed[0:count // 2 * 2:2], mixed[1:count // 2 * 2:2]
    margin = jnp.minimum(tallies[source_of] - 1, limit - tallies[sink]) // 2
    margin = jnp.where((source_of == sequence[0]) | (sink == sequence[0]) | (tallies[sink] == 0), 0, jnp.maximum(margin, 0))
    moved = jax.random.randint(jax.random.fold_in(own, 4), (count // 2,), 0, 1 << 20) % (margin + 1)
    tallies = tallies.at[source_of].add(-moved).at[sink].add(moved)
    members = jnp.searchsorted(jnp.cumsum(tallies), jnp.arange(rows * top), side="right").astype(jnp.int32)
    grid = members.reshape(top, rows).T
    grid = grid[jax.random.permutation(jax.random.fold_in(own, 1), rows)]
    rotation = jax.random.randint(jax.random.fold_in(own, 2), (rows, 1), 0, top)
    return jnp.take_along_axis(grid, (jnp.arange(top)[None, :] + rotation) % top, axis=1)


def portions_of(amount, total, reach, slope, full):
    weights = [(1 << 20) // math.isqrt(grade ** slope) + 1 for grade in range(1, amount + 1)]
    largest = reach if full else min(reach, max(-(-total // amount), total * weights[0] // sum(weights)))
    least = 1 if total - largest >= amount - 1 else 0
    given, surplus = [largest] + [least] * (amount - 1), total - largest - least * (amount - 1)
    while surplus > 0:
        free = [i for i in range(1, amount) if given[i] < largest] or [i for i in range(1, amount) if given[i] < reach]
        whole, budget = sum([weights[i] for i in free]), surplus
        for i in free:
            extra = min(reach - given[i], max(1, budget * weights[i] // whole), surplus)
            given[i] = given[i] + extra
            surplus = surplus - extra
    return np.array(given)


def scatter_about(key, dims, deviation, bound, cuts=(), kind=jnp.bfloat16):
    drawn = deviation * jax.random.normal(key, dims, jnp.float32)
    if cuts:
        drawn = drawn * steps_of(key, dims, cuts, -0.22, 0.18)
    return jnp.clip(drawn, -bound, bound).astype(kind)


def setup_inputs(seed: int = 0) -> dict:
    key_of = jax.random.split(jax.random.key(seed), 21)
    tokens = scatter_about(key_of[0], (TOKENS, D), 1.0, 6.0, ((0, 16),))
    norm_attn = jnp.clip(1.0 + 0.18 * jax.random.normal(key_of[1], (D,), jnp.float32), 0.1, 1.9)
    w_query = scatter_about(key_of[2], (D, HEADS * HEAD_DIM), D ** -0.5, 0.125, ((1, 2),))
    w_key = scatter_about(key_of[3], (D, KV_HEADS * HEAD_DIM), D ** -0.5, 0.125, ((1, 2),))
    w_value = scatter_about(key_of[4], (D, KV_HEADS * HEAD_DIM), D ** -0.5, 0.125, ((1, 2),))
    w_out = scatter_about(key_of[5], (HEADS * HEAD_DIM, D), (HEADS * HEAD_DIM) ** -0.5, 0.125, ((0, 2),))
    attn_bias = jnp.clip(-7.0 + 6.0 * jax.random.uniform(key_of[6], (HEADS,), jnp.float32) ** steps_of(key_of[6], (HEADS,), ((0, 2),), -0.2, 0.2), -7.0, -1.0)
    cache_keys = scatter_about(key_of[7], (TOKENS, CACHE, KV_HEADS * HEAD_DIM), 1.0, 6.0, ((0, 16), (2, 2)))
    cache_values = scatter_about(key_of[8], (TOKENS, CACHE, KV_HEADS * HEAD_DIM), 1.0, 6.0, ((0, 16), (2, 2)))
    lengths = place_ends(jax.random.randint(key_of[9], (TOKENS,), CACHE // 4, CACHE + 1), jax.random.fold_in(key_of[9], 1), CACHE // 4, CACHE).astype(jnp.int32)
    norm_ffn = jnp.clip(1.0 + 0.18 * jax.random.normal(key_of[10], (D,), jnp.float32), 0.1, 1.9)
    expert_gate = scatter_about(key_of[11], (D, EXPERTS * FF), D ** -0.5, 0.125, ((1, 32),))
    expert_up = scatter_about(key_of[12], (D, EXPERTS * FF), D ** -0.5, 0.125, ((1, 32),))
    expert_down = scatter_about(key_of[13], (EXPERTS * FF, D), FF ** -0.5, 0.0625, ((0, 32),))
    dense_gate_w = scatter_about(key_of[14], (D, DENSE_FF), D ** -0.5, 0.125, ((1, 16),))
    dense_up_w = scatter_about(key_of[15], (D, DENSE_FF), D ** -0.5, 0.125, ((1, 16),))
    dense_down_w = scatter_about(key_of[16], (DENSE_FF, D), DENSE_FF ** -0.5, 0.0625, ((0, 16),))
    dense_mix = scatter_about(key_of[17], (D,), D ** -0.5, 0.125)
    routes_keys = jax.random.split(jax.random.fold_in(key_of[18], 1), TOKENS // ROWS_DEV)
    routes_turns = jax.random.permutation(jax.random.fold_in(key_of[18], 3), TOKENS // ROWS_DEV)
    routes = jax.vmap(lambda own, number: assign_block(jax.random.fold_in(key_of[18], 2), own, number, ROWS_DEV, EXPERTS, TOP, CAP_DEV, 1))(routes_keys, routes_turns).reshape((TOKENS, TOP))
    route_weights = jnp.clip(jnp.exp(math.log(1.0) - 1.6133518 * jax.random.uniform(key_of[19], (TOKENS, TOP), jnp.float32) ** steps_of(key_of[19], (TOKENS, TOP), ((0, 32),), -0.2, 0.2)), 0.19921875, 1.0).astype(jnp.bfloat16)
    return {"tokens": tokens, "norm_attn": norm_attn, "w_query": w_query, "w_key": w_key, "w_value": w_value, "w_out": w_out, "attn_bias": attn_bias, "cache_keys": cache_keys, "cache_values": cache_values, "lengths": lengths, "norm_ffn": norm_ffn, "expert_gate": expert_gate, "expert_up": expert_up, "expert_down": expert_down, "dense_gate_w": dense_gate_w, "dense_up_w": dense_up_w, "dense_down_w": dense_down_w, "dense_mix": dense_mix, "routes": routes, "route_weights": route_weights}


EPSILON = 1e-06

def normed_rows(values, gain):
    widened = values.astype(jnp.float32)
    scale = lax.rsqrt(lax.optimization_barrier(jnp.mean(widened * widened, axis=-1, keepdims=True)) + EPSILON)
    return (widened * scale * gain).astype(jnp.bfloat16)

def reference(tokens, norm_attn, w_query, w_key, w_value, w_out, attn_bias, cache_keys, cache_values, lengths, norm_ffn, expert_gate, expert_up, expert_down, dense_gate_w, dense_up_w, dense_down_w, dense_mix, routes, route_weights):
    repeat = HEADS // KV_HEADS
    normed = normed_rows(tokens, norm_attn)
    query = jnp.dot(normed, w_query, preferred_element_type=jnp.float32).astype(jnp.bfloat16)
    new_keys = jnp.dot(normed, w_key, preferred_element_type=jnp.float32).astype(jnp.bfloat16)
    new_values = jnp.dot(normed, w_value, preferred_element_type=jnp.float32).astype(jnp.bfloat16)
    offsets = attn_bias.reshape(KV_HEADS, repeat)

    def attend(block):
        query_block, key_block, value_block, length_block = block
        query_heads = query_block.astype(jnp.float32).reshape(SEQS_DEV, KV_HEADS, repeat, HEAD_DIM)
        key_heads = key_block.astype(jnp.float32).reshape(SEQS_DEV, CACHE, KV_HEADS, HEAD_DIM)
        value_heads = value_block.astype(jnp.float32).reshape(SEQS_DEV, CACHE, KV_HEADS, HEAD_DIM)
        scores = jnp.einsum('bgrd,bsgd->bgrs', query_heads, key_heads) * HEAD_DIM ** (-0.5)
        scores = scores + offsets[None, :, :, None]
        places = lax.broadcasted_iota(jnp.int32, (SEQS_DEV, CACHE), 1)
        visible = (places < length_block[:, None])[:, None, None, :]
        log_keep = jnp.where(visible, jax.nn.log_sigmoid(-scores), 0.0)
        after = lax.cumsum(log_keep, axis=3, reverse=True) - log_keep
        weight = jnp.where(visible, jnp.exp(jax.nn.log_sigmoid(scores) + after), 0.0).astype(jnp.bfloat16)
        mixed = jnp.einsum('bgrs,bsgd->bgrd', weight.astype(jnp.float32), value_heads)
        return mixed.astype(jnp.bfloat16).reshape(SEQS_DEV, HEADS * HEAD_DIM)
    heads_out = lax.map(attend, (query.reshape(N_EP, SEQS_DEV, HEADS * HEAD_DIM), cache_keys.reshape(N_EP, SEQS_DEV, CACHE, KV_HEADS * HEAD_DIM), cache_values.reshape(N_EP, SEQS_DEV, CACHE, KV_HEADS * HEAD_DIM), lengths.reshape(N_EP, SEQS_DEV))).reshape(TOKENS, HEADS * HEAD_DIM)
    run_width = HEADS * HEAD_DIM // N_TP
    attn_sum = jnp.zeros((TOKENS, D), jnp.float32)
    for run in range(N_TP):
        partial_value = jnp.dot(heads_out[:, run * run_width:(run + 1) * run_width], w_out[run * run_width:(run + 1) * run_width], preferred_element_type=jnp.float32)
        attn_sum = attn_sum + lax.optimization_barrier(partial_value.astype(jnp.bfloat16)).astype(jnp.float32)
    middle = (tokens.astype(jnp.float32) + attn_sum).astype(jnp.bfloat16)
    normed_two = normed_rows(middle, norm_ffn)
    mix_gate = jax.nn.sigmoid(jnp.dot(normed_two, dense_mix, preferred_element_type=jnp.float32))
    dense_hidden = (jax.nn.silu(jnp.dot(normed_two, dense_gate_w, preferred_element_type=jnp.float32)) * jnp.dot(normed_two, dense_up_w, preferred_element_type=jnp.float32)).astype(jnp.bfloat16)
    dense_term = jnp.dot(dense_hidden, dense_down_w, preferred_element_type=jnp.float32) * mix_gate[:, None]
    sources = N_EP * N_TP
    route_blocks = routes.reshape(sources, ROWS_DEV, TOP)
    weight_blocks = route_weights.astype(jnp.float32).reshape(sources, ROWS_DEV, TOP)
    row_blocks = normed_two.astype(jnp.float32).reshape(sources, ROWS_DEV, D)
    slot_ids = lax.broadcasted_iota(jnp.int32, (sources, CAP_DEV, ROWS_DEV), 1)

    def one_expert(expert_id):
        matched = route_blocks == expert_id
        present = jnp.any(matched, axis=2).astype(jnp.int32)
        share = lax.optimization_barrier(jnp.sum(jnp.where(matched, weight_blocks, 0.0), axis=2))
        ranks = jnp.cumsum(present, axis=1) - 1
        selector = ((present[:, None, :] == 1) & (ranks[:, None, :] == slot_ids)).astype(jnp.float32)
        slot_rows = jnp.einsum('dcr,drk->dck', selector, row_blocks).astype(jnp.bfloat16).reshape(sources * CAP_DEV, D)
        start = (expert_id * FF).astype(jnp.int32)
        gate_cols = lax.dynamic_slice_in_dim(expert_gate, start, FF, 1)
        up_cols = lax.dynamic_slice_in_dim(expert_up, start, FF, 1)
        down_rows = lax.dynamic_slice_in_dim(expert_down, start, FF, 0)
        hidden = (jax.nn.silu(jnp.dot(slot_rows, gate_cols, preferred_element_type=jnp.float32)) * jnp.dot(slot_rows, up_cols, preferred_element_type=jnp.float32)).astype(jnp.bfloat16)
        result = jnp.dot(hidden, down_rows, preferred_element_type=jnp.float32).reshape(sources, CAP_DEV, D)
        returned = jnp.einsum('dcr,dck->drk', selector, result) * share[:, :, None]
        return returned.reshape(TOKENS, D)
    expert_term = lax.optimization_barrier(jnp.sum(lax.map(one_expert, jnp.arange(EXPERTS, dtype=jnp.int32)), axis=0))
    layer_out = (middle.astype(jnp.float32) + expert_term + dense_term).astype(jnp.bfloat16)
    return (layer_out, new_keys, new_values)
```

```python
import functools

import jax
import jax.numpy as jnp
from jax import lax
from jax.experimental import pallas as pl
from jax.experimental.pallas import tpu as pltpu
from jax.sharding import PartitionSpec as P

HEAD_DIM = 64
EXPERTS = 8
TOP = 2
EPSILON = 1e-06
LANES = 128
MESH = pl.DeviceIdType.MESH
F32 = jnp.float32
BF16 = jnp.bfloat16


def dot(a, b, dims=((1,), (0,))):
    return lax.dot_general(a, b, (dims, ((), ())), preferred_element_type=F32)


def normed_rows(widened, gain):
    scale = lax.rsqrt(jnp.mean(widened * widened, axis=-1, keepdims=True) + EPSILON)
    return (widened * scale * gain).astype(BF16)


def tile_of(size):
    for tile in (256, 128):
        if size % tile == 0:
            return tile
    return size


def tiled(size, body):
    tile = tile_of(size)
    if tile == size:
        body(pl.ds(0, size))
        return

    def step(i, carry):
        body(pl.ds(pl.multiple_of(i * tile, tile), tile))
        return carry

    lax.fori_loop(0, size // tile, step, 0)


def kernel(
    n_ep, n_tp,
    tokens, norm_attn, bias, lengths, norm_ffn, mix, share,
    wq_hbm, wk_hbm, wv_hbm, wo_hbm, ck_hbm, cv_hbm, eg_hbm, eu_hbm, ed_hbm, dg_hbm, du_hbm, dd_hbm,
    out, new_keys, new_values,
    wq, wk, wv, wo, ck, cv, eg, eu, ed, dg, du, dd,
    q_heads, o_heads, flat, pair_out, pair_in, own_tokens,
    gathered, shares, slots, e_hidden, d_hidden, mine, theirs_out, theirs_in, sums, scatter_out, scatter_in,
    w_sem, k_sem, v_sem, pair_sem, g_send, g_recv, s_send, s_recv, slot_sem, back_sem, r_send, r_recv,
):
    ep, tp = lax.axis_index("ep"), lax.axis_index("tp")
    other = 1 - tp
    seqs, width = tokens.shape
    rows = seqs // n_tp
    cache_len = ck.shape[1]
    heads = bias.shape[0]
    tiles = heads * HEAD_DIM // LANES
    half = heads // 2
    cap = slots.shape[1] // n_ep
    n_rows = n_ep * rows

    barrier = pltpu.get_barrier_semaphore()

    def greet(k, carry):
        peer = lax.rem(ep + k, n_ep)
        pl.semaphore_signal(barrier, inc=1, device_id=(peer, tp), device_id_type=MESH)
        return carry

    pl.semaphore_signal(barrier, inc=1, device_id=(ep, other), device_id_type=MESH)
    lax.fori_loop(1, n_ep, greet, 0)

    pairs = [(wq_hbm, wq), (wk_hbm, wk), (wv_hbm, wv), (wo_hbm, wo), (dg_hbm, dg), (du_hbm, du),
             (eg_hbm, eg), (eu_hbm, eu), (ed_hbm, ed), (dd_hbm, dd)]
    loads = [pltpu.make_async_copy(a, b, w_sem.at[i]) for i, (a, b) in enumerate(pairs)]
    l_wq, l_wk, l_wv, l_wo, l_dg, l_du, l_eg, l_eu, l_ed, l_dd = loads

    def key_load(b):
        return pltpu.make_async_copy(ck_hbm.at[b], ck.at[b], k_sem.at[b])

    def value_load(b):
        return pltpu.make_async_copy(cv_hbm.at[b], cv.at[b], v_sem.at[b])

    l_wq.start()
    l_wk.start()
    l_wv.start()

    def start_cache(b, carry):
        key_load(b).start()
        value_load(b).start()
        return carry

    lax.fori_loop(0, seqs, start_cache, 0)
    for load in (l_wo, l_dg, l_du, l_eg, l_eu, l_ed, l_dd):
        load.start()

    widened = tokens[...].astype(F32)
    own_tokens[...] = widened.reshape(n_tp, rows, width)
    normed = normed_rows(widened, norm_attn[...])
    l_wq.wait()
    lane = lax.broadcasted_iota(jnp.int32, (seqs, LANES), 1)
    low = lane < HEAD_DIM
    for j in range(tiles):
        tile = dot(normed, wq[:, j * LANES:(j + 1) * LANES]).astype(BF16).astype(F32)
        rolled = pltpu.roll(tile, HEAD_DIM, 1)
        for side in range(2):
            head = 2 * j + side
            group = head // half
            value = tile if side == group else rolled
            q_heads[:, head, :] = jnp.where(low if group == 0 else ~low, value, 0.0)
    l_wk.wait()
    new_keys[...] = dot(normed, wk[...]).astype(BF16)
    l_wv.wait()
    new_values[...] = dot(normed, wv[...]).astype(BF16)

    blocks = cache_len // LANES
    tri = (
        lax.broadcasted_iota(jnp.int32, (LANES, LANES), 0)
        > lax.broadcasted_iota(jnp.int32, (LANES, LANES), 1)
    ).astype(F32).astype(BF16)
    places = lax.broadcasted_iota(jnp.int32, (heads, cache_len), 1)
    offsets = bias[...]

    def attend(b):
        key_load(b).wait()
        query = q_heads[b].astype(BF16)
        z = dot(query, ck[b], ((1,), (1,))) * HEAD_DIM ** (-0.5) + offsets
        visible = places < lengths[b]
        soft = jnp.log(1.0 + jnp.exp(-jnp.abs(z)))
        take = jnp.minimum(z, 0.0) - soft
        keep = jnp.where(visible, jnp.minimum(-z, 0.0) - soft, 0.0)
        stack = jnp.concatenate([keep[:, n * LANES:(n + 1) * LANES] for n in range(blocks)], axis=0)
        high = stack.astype(BF16)
        rest = (stack - high.astype(F32)).astype(BF16)
        within = dot(high, tri) + dot(rest, tri)
        totals = jnp.sum(stack, axis=1, keepdims=True)
        carry = jnp.zeros((heads, 1), F32)
        after = [None] * blocks
        for n in range(blocks - 1, -1, -1):
            after[n] = within[n * heads:(n + 1) * heads] + carry
            carry = carry + totals[n * heads:(n + 1) * heads]
        weight = jnp.where(visible, jnp.exp(take + jnp.concatenate(after, axis=1)), 0.0).astype(BF16)
        value_load(b).wait()
        o_heads[b] = dot(weight, cv[b]).astype(BF16).astype(F32)

    step_seqs = 2 if seqs % 2 == 0 else 1

    def attend_step(t, carry):
        for i in range(step_seqs):
            attend(t * step_seqs + i)
        return carry

    lax.fori_loop(0, seqs // step_seqs, attend_step, 0)

    for j in range(tiles):
        first, second = o_heads[:, 2 * j, :], o_heads[:, 2 * j + 1, :]
        if 2 * j < half:
            second = pltpu.roll(second, HEAD_DIM, 1)
        else:
            first = pltpu.roll(first, HEAD_DIM, 1)
        flat[:, j * LANES:(j + 1) * LANES] = jnp.where(low, first, second).astype(BF16)
    l_wo.wait()

    def project(cols):
        value = dot(flat[...], wo[:, cols]).astype(BF16).astype(F32)
        pair_out[:, :, cols] = value.reshape(n_tp, rows, value.shape[1])

    tiled(width, project)

    pl.semaphore_wait(barrier, n_ep)
    pair_copy = pltpu.make_async_remote_copy(
        pair_out.at[other], pair_in, pair_sem.at[0], pair_sem.at[1],
        device_id=(ep, other), device_id_type=MESH)
    pair_copy.start()
    shares[ep] = share[...]
    pair_copy.wait_recv()
    middle = (own_tokens[tp] + (pair_out[tp] + pair_in[...])).astype(BF16).astype(F32)
    gathered[ep] = normed_rows(middle, norm_ffn[...])

    def gather_copy(dest, block, index):
        return pltpu.make_async_remote_copy(
            gathered.at[block], gathered.at[block], g_send.at[index], g_recv.at[block],
            device_id=(dest, tp), device_id_type=MESH)

    def share_copy(dest, block, index):
        return pltpu.make_async_remote_copy(
            share, shares.at[block], s_send.at[index], s_recv.at[block],
            device_id=(dest, tp), device_id_type=MESH)

    def send_rows(k, carry):
        dest = lax.rem(ep + k, n_ep)
        share_copy(dest, ep, dest).start()
        gather_copy(dest, ep, dest).start()
        return carry

    def await_rows(k, carry):
        source = lax.rem(ep + k, n_ep)
        share_copy(source, source, source).wait_recv()
        gather_copy(source, source, source).wait_recv()
        return carry

    lax.fori_loop(1, n_ep, send_rows, 0)
    lax.fori_loop(1, n_ep, await_rows, 0)

    everything = gathered[...].astype(F32).reshape(n_rows, width)
    mix_gate = jax.nn.sigmoid(jnp.sum(everything * mix[...], axis=1, keepdims=True))
    everything = everything.astype(BF16)

    members = n_ep * n_tp // EXPERTS
    expert = (ep * n_tp + tp) // members
    share_all = shares[...].reshape(n_rows, LANES).astype(BF16)
    one_hot = (lax.broadcasted_iota(jnp.int32, (8, LANES), 1) == expert).astype(F32).astype(BF16)
    share_row = dot(one_hot, share_all, ((1,), (1,)))
    present = (share_row > 0.0).astype(F32)
    row_j = lax.broadcasted_iota(jnp.int32, (n_rows, n_rows), 0)
    row_i = lax.broadcasted_iota(jnp.int32, (n_rows, n_rows), 1)
    shift = rows.bit_length() - 1
    same = ((row_j >> shift) == (row_i >> shift)) & (row_j <= row_i)
    rank = dot(present.astype(BF16), same.astype(F32).astype(BF16)) - 1.0
    n_slots = n_ep * cap
    slot = lax.broadcasted_iota(jnp.int32, (n_slots, n_rows), 0)
    block = lax.broadcasted_iota(jnp.int32, (n_slots, n_rows), 1) >> shift
    picked = ((slot - cap * block).astype(F32) == rank[0:1]) & (present[0:1] > 0.0)
    selector = picked.astype(F32)
    slot_share = jnp.sum(selector * share_row[0:1], axis=1, keepdims=True)
    selector = selector.astype(BF16)
    slots[0] = dot(selector, everything).astype(BF16)
    slot_copy = pltpu.make_async_remote_copy(
        slots.at[0], slots.at[1], slot_sem.at[0], slot_sem.at[1],
        device_id=(ep, other), device_id_type=MESH)
    slot_copy.start()

    l_dg.wait()
    l_du.wait()

    def dense_up(cols):
        up = dot(everything, du[:, cols])
        d_hidden[:, cols] = (jax.nn.silu(dot(everything, dg[:, cols])) * up).astype(BF16)

    tiled(d_hidden.shape[1], dense_up)

    l_eg.wait()
    l_eu.wait()
    slot_copy.wait_recv()
    slot_rows = slots[...].reshape(2 * n_slots, width)

    def expert_up(cols):
        up = dot(slot_rows, eu[:, cols])
        e_hidden[:, cols] = (jax.nn.silu(dot(slot_rows, eg[:, cols])) * up).astype(BF16)

    tiled(e_hidden.shape[1], expert_up)
    l_ed.wait()

    def expert_down(cols):
        value = dot(e_hidden[...], ed[:, cols])
        mine[:, cols] = value[:n_slots]
        theirs_out[:, cols] = value[n_slots:].astype(BF16)

    tiled(width, expert_down)
    back_copy = pltpu.make_async_remote_copy(
        theirs_out, theirs_in, back_sem.at[0], back_sem.at[1],
        device_id=(ep, other), device_id_type=MESH)
    back_copy.start()
    l_dd.wait()

    def dense_down(cols):
        sums[:, cols] = dot(d_hidden[...], dd[:, cols]) * mix_gate

    tiled(width, dense_down)
    back_copy.wait_recv()

    def combine(cols):
        result = ((mine[:, cols] + theirs_in[:, cols].astype(F32)) * slot_share).astype(BF16)
        total = sums[:, cols] + dot(selector, result, ((0,), (0,)))
        scatter_out[:, :, cols] = total.reshape(n_ep, rows, total.shape[1]).astype(BF16)

    tiled(width, combine)

    def scatter_copy(dest, source):
        return pltpu.make_async_remote_copy(
            scatter_out.at[dest], scatter_in.at[source], r_send.at[dest], r_recv.at[source],
            device_id=(dest, tp), device_id_type=MESH)

    def send_sums(k, carry):
        dest = lax.rem(ep + k, n_ep)
        scatter_copy(dest, ep).start()
        return carry

    lax.fori_loop(1, n_ep, send_sums, 0)

    def add_sums(k, total):
        source = lax.rem(ep + n_ep - k, n_ep)
        scatter_copy(source, source).wait_recv()
        return total + scatter_in[source].astype(F32)

    total = lax.fori_loop(1, n_ep, add_sums, middle + scatter_out[ep].astype(F32))
    out[...] = total.astype(BF16)

    pair_copy.wait_send()
    slot_copy.wait_send()
    back_copy.wait_send()

    def finish(k, carry):
        dest = lax.rem(ep + k, n_ep)
        share_copy(dest, ep, dest).wait_send()
        gather_copy(dest, ep, dest).wait_send()
        scatter_copy(dest, ep).wait_send()
        return carry

    lax.fori_loop(1, n_ep, finish, 0)


def shards(
    n_ep, n_tp,
    tokens, norm_attn, w_query, w_key, w_value, w_out, attn_bias, cache_keys, cache_values, lengths,
    norm_ffn, expert_gate, expert_up, expert_down, dense_gate_w, dense_up_w, dense_down_w, dense_mix,
    routes, route_weights,
):
    seqs, width = tokens.shape
    rows = seqs // n_tp
    heads = attn_bias.shape[0]
    cap = (rows * TOP + EXPERTS - 1) // EXPERTS + 1
    ids = lax.broadcasted_iota(jnp.int32, (1, 1, LANES), 2)
    matched = routes[:, :, None] == ids
    share = jnp.sum(jnp.where(matched, route_weights.astype(F32)[:, :, None], 0.0), axis=1)
    weights = (w_query, w_key, w_value, w_out, cache_keys, cache_values, expert_gate, expert_up,
               expert_down, dense_gate_w, dense_up_w, dense_down_w)
    vmem = pl.BlockSpec(memory_space=pltpu.VMEM)
    smem = pl.BlockSpec(memory_space=pltpu.SMEM)
    hbm = pl.BlockSpec(memory_space=pl.ANY)
    n_slots = n_ep * cap
    ff, dense_ff = expert_gate.shape[1], dense_gate_w.shape[1]
    dma = pltpu.SemaphoreType.DMA
    scratch = [pltpu.VMEM(w.shape, w.dtype) for w in weights] + [
        pltpu.VMEM((seqs, heads, LANES), F32),
        pltpu.VMEM((seqs, heads, LANES), F32),
        pltpu.VMEM((seqs, heads * HEAD_DIM), BF16),
        pltpu.VMEM((n_tp, rows, width), F32),
        pltpu.VMEM((rows, width), F32),
        pltpu.VMEM((n_tp, rows, width), F32),
        pltpu.VMEM((n_ep, rows, width), BF16),
        pltpu.VMEM((n_ep, rows, LANES), F32),
        pltpu.VMEM((2, n_slots, width), BF16),
        pltpu.VMEM((2 * n_slots, ff), BF16),
        pltpu.VMEM((n_ep * rows, dense_ff), BF16),
        pltpu.VMEM((n_slots, width), F32),
        pltpu.VMEM((n_slots, width), BF16),
        pltpu.VMEM((n_slots, width), BF16),
        pltpu.VMEM((n_ep * rows, width), F32),
        pltpu.VMEM((n_ep, rows, width), BF16),
        pltpu.VMEM((n_ep, rows, width), BF16),
        dma((10,)), dma((seqs,)), dma((seqs,)), dma((2,)),
        dma((n_ep,)), dma((n_ep,)), dma((n_ep,)), dma((n_ep,)),
        dma((2,)), dma((2,)), dma((n_ep,)), dma((n_ep,)),
    ]
    return pl.pallas_call(
        functools.partial(kernel, n_ep, n_tp),
        out_shape=(
            jax.ShapeDtypeStruct((rows, width), BF16),
            jax.ShapeDtypeStruct((seqs, w_key.shape[1]), BF16),
            jax.ShapeDtypeStruct((seqs, w_value.shape[1]), BF16),
        ),
        in_specs=[vmem, vmem, vmem, smem, vmem, vmem, vmem] + [hbm] * 12,
        out_specs=(vmem, vmem, vmem),
        scratch_shapes=scratch,
        compiler_params=pltpu.CompilerParams(
            collective_id=0, has_side_effects=True, vmem_limit_bytes=67043328
        ),
    )(tokens, norm_attn[None], attn_bias[:, None], lengths, norm_ffn[None],
      dense_mix.astype(F32)[None], share, *weights)


def solution(mesh):
    placed = (
        P("ep", None),
        P(),
        P(None, "tp"),
        P(None, "tp"),
        P(None, "tp"),
        P("tp", None),
        P("tp"),
        P("ep", None, "tp"),
        P("ep", None, "tp"),
        P("ep"),
        P(),
        P(None, ("ep", "tp")),
        P(None, ("ep", "tp")),
        P(("ep", "tp"), None),
        P(None, "ep"),
        P(None, "ep"),
        P("ep", None),
        P(),
        P(("ep", "tp"), None),
        P(("ep", "tp"), None),
    )
    return jax.shard_map(
        functools.partial(shards, mesh.shape["ep"], mesh.shape["tp"]),
        mesh=mesh,
        in_specs=placed,
        out_specs=(P(("ep", "tp"), None), P("ep", "tp"), P("ep", "tp")),
        check_vma=False,
    )
```

```python
import functools

import jax
import jax.numpy as jnp
from jax import lax
from jax.experimental import pallas as pl
from jax.experimental.pallas import tpu as pltpu
from jax.sharding import PartitionSpec as P

HEAD_DIM = 64
EXPERTS = 8
TOP = 2
EPSILON = 1e-06
LANES = 128
MESH = pl.DeviceIdType.MESH
F32 = jnp.float32
BF16 = jnp.bfloat16


def dot(a, b, dims=((1,), (0,))):
    return lax.dot_general(a, b, (dims, ((), ())), preferred_element_type=F32)


def normed_rows(widened, gain):
    scale = lax.rsqrt(jnp.mean(widened * widened, axis=-1, keepdims=True) + EPSILON)
    return (widened * scale * gain).astype(BF16)


def tile_of(size):
    for tile in (256, 128):
        if size % tile == 0:
            return tile
    return size


def tiled(size, body, start=0):
    tile = tile_of(size)
    if tile == size:
        body(pl.ds(start, size))
        return

    def step(i, carry):
        body(pl.ds(pl.multiple_of(i * tile + start, tile), tile))
        return carry

    lax.fori_loop(0, size // tile, step, 0)


def kernel(
    n_ep, n_tp,
    tokens, norm_attn, bias, lengths, norm_ffn, mix, routes, route_weights,
    wq_hbm, wk_hbm, wv_hbm, wo_hbm, ck_hbm, cv_hbm, eg_hbm, eu_hbm, ed_hbm, dg_hbm, du_hbm, dd_hbm,
    out, new_keys, new_values,
    wq, wk, wv, wo, ck, cv, eg, eu, ed, dg, du, dd,
    q_heads, o_heads, flat, pair_out, pair_in, own_tokens, share,
    gathered, shares, slots, e_hidden, d_hidden, mine, theirs_out, theirs_in, scatter_out, scatter_in,
    w_sem, k_sem, v_sem, pair_sem, g_send, g_recv, s_send, s_recv, slot_sem, back_sem, r_send, r_recv,
):
    ep, tp = lax.axis_index("ep"), lax.axis_index("tp")
    other = 1 - tp
    seqs, width = tokens.shape
    rows = seqs // n_tp
    cache_len = ck.shape[1]
    heads = bias.shape[0]
    tiles = heads * HEAD_DIM // LANES
    half = heads // 2
    cap = slots.shape[1] // n_ep
    n_rows = n_ep * rows

    barrier = pltpu.get_barrier_semaphore()

    def greet(k, carry):
        peer = lax.rem(ep + k, n_ep)
        pl.semaphore_signal(barrier, inc=1, device_id=(peer, tp), device_id_type=MESH)
        return carry

    pl.semaphore_signal(barrier, inc=1, device_id=(ep, other), device_id_type=MESH)
    lax.fori_loop(1, n_ep, greet, 0)

    pairs = [(wq_hbm, wq), (wk_hbm, wk), (wv_hbm, wv), (wo_hbm, wo), (dg_hbm, dg), (du_hbm, du),
             (eg_hbm, eg), (eu_hbm, eu), (ed_hbm, ed), (dd_hbm, dd)]
    loads = [pltpu.make_async_copy(a, b, w_sem.at[i]) for i, (a, b) in enumerate(pairs)]
    l_wq, l_wk, l_wv, l_wo, l_dg, l_du, l_eg, l_eu, l_ed, l_dd = loads

    def key_load(b):
        return pltpu.make_async_copy(ck_hbm.at[b], ck.at[b], k_sem.at[b])

    def value_load(b):
        return pltpu.make_async_copy(cv_hbm.at[b], cv.at[b], v_sem.at[b])

    l_wq.start()
    l_wk.start()
    l_wv.start()

    def start_cache(b, carry):
        key_load(b).start()
        value_load(b).start()
        return carry

    lax.fori_loop(0, seqs, start_cache, 0)
    for load in (l_wo, l_dg, l_du, l_eg, l_eu, l_ed, l_dd):
        load.start()

    ids = lax.broadcasted_iota(jnp.int32, (LANES, rows), 0)
    share_columns = jnp.zeros((LANES, rows), F32)
    for choice in range(TOP):
        chosen = ids == routes[choice:choice + 1, :]
        value = route_weights[choice:choice + 1, :].astype(F32)
        share_columns = share_columns + jnp.where(chosen, value, 0.0)
    diagonal = (
        lax.broadcasted_iota(jnp.int32, (rows, rows), 0) == lax.broadcasted_iota(jnp.int32, (rows, rows), 1)
    ).astype(F32).astype(BF16)
    share[...] = dot(diagonal, share_columns.astype(BF16), ((1,), (1,)))

    widened = tokens[...].astype(F32)
    own_tokens[...] = widened.reshape(n_tp, rows, width)
    normed = normed_rows(widened, norm_attn[...])
    l_wq.wait()
    lane = lax.broadcasted_iota(jnp.int32, (seqs, LANES), 1)
    low = lane < HEAD_DIM
    for j in range(tiles):
        tile = dot(normed, wq[:, j * LANES:(j + 1) * LANES]).astype(BF16).astype(F32)
        rolled = pltpu.roll(tile, HEAD_DIM, 1)
        for side in range(2):
            head = 2 * j + side
            group = head // half
            value = tile if side == group else rolled
            q_heads[:, head, :] = jnp.where(low if group == 0 else ~low, value, 0.0)
    l_wk.wait()
    new_keys[...] = dot(normed, wk[...]).astype(BF16)
    l_wv.wait()
    new_values[...] = dot(normed, wv[...]).astype(BF16)

    blocks = cache_len // LANES
    tri = (
        lax.broadcasted_iota(jnp.int32, (LANES, LANES), 0)
        > lax.broadcasted_iota(jnp.int32, (LANES, LANES), 1)
    ).astype(F32).astype(BF16)
    places = lax.broadcasted_iota(jnp.int32, (heads, cache_len), 1)
    head_ids = lax.broadcasted_iota(jnp.int32, (heads, LANES), 0)
    offsets = jnp.zeros((heads, LANES), F32)
    for head in range(heads):
        offsets = jnp.where(head_ids == head, bias[head], offsets)
    offsets = jnp.concatenate([offsets] * blocks, axis=1)

    def attend(b):
        query = q_heads[b].astype(BF16)
        z = dot(query, ck[b], ((1,), (1,))) * HEAD_DIM ** (-0.5) + offsets
        visible = places < lengths[b]
        soft = jnp.log(1.0 + jnp.exp(-jnp.abs(z)))
        take = jnp.minimum(z, 0.0) - soft
        keep = jnp.where(visible, jnp.minimum(-z, 0.0) - soft, 0.0)
        stack = jnp.concatenate([keep[:, n * LANES:(n + 1) * LANES] for n in range(blocks)], axis=0)
        high = stack.astype(BF16)
        rest = (stack - high.astype(F32)).astype(BF16)
        within = dot(high, tri) + dot(rest, tri)
        totals = jnp.sum(stack, axis=1, keepdims=True)
        carry = jnp.zeros((heads, 1), F32)
        after = [None] * blocks
        for n in range(blocks - 1, -1, -1):
            after[n] = within[n * heads:(n + 1) * heads] + carry
            carry = carry + totals[n * heads:(n + 1) * heads]
        weight = jnp.where(visible, jnp.exp(take + jnp.concatenate(after, axis=1)), 0.0).astype(BF16)
        return dot(weight, cv[b]).astype(BF16).astype(F32)

    step_seqs = 4 if seqs % 4 == 0 else 1

    def attend_step(t, carry):
        for i in range(step_seqs):
            key_load(t * step_seqs + i).wait()
            value_load(t * step_seqs + i).wait()
        mixed = [attend(t * step_seqs + i) for i in range(step_seqs)]
        for i in range(step_seqs):
            o_heads[t * step_seqs + i] = mixed[i]
        return carry

    lax.fori_loop(0, seqs // step_seqs, attend_step, 0)

    for j in range(tiles):
        first, second = o_heads[:, 2 * j, :], o_heads[:, 2 * j + 1, :]
        if 2 * j < half:
            second = pltpu.roll(second, HEAD_DIM, 1)
        else:
            first = pltpu.roll(first, HEAD_DIM, 1)
        flat[:, j * LANES:(j + 1) * LANES] = jnp.where(low, first, second).astype(BF16)
    l_wo.wait()

    def project(cols):
        value = dot(flat[...], wo[:, cols]).astype(BF16).astype(F32)
        pair_out[:, :, cols] = value.reshape(n_tp, rows, value.shape[1])

    tiled(width, project)

    pl.semaphore_wait(barrier, n_ep)
    pair_copy = pltpu.make_async_remote_copy(
        pair_out.at[other], pair_in, pair_sem.at[0], pair_sem.at[1],
        device_id=(ep, other), device_id_type=MESH)
    pair_copy.start()
    shares[ep] = share[...]
    pair_copy.wait_recv()
    middle = (own_tokens[tp] + (pair_out[tp] + pair_in[...])).astype(BF16).astype(F32)
    gathered[ep] = normed_rows(middle, norm_ffn[...])

    def gather_copy(dest, block, index):
        return pltpu.make_async_remote_copy(
            gathered.at[block], gathered.at[block], g_send.at[index], g_recv.at[block],
            device_id=(dest, tp), device_id_type=MESH)

    def share_copy(dest, block, index):
        return pltpu.make_async_remote_copy(
            share, shares.at[block], s_send.at[index], s_recv.at[block],
            device_id=(dest, tp), device_id_type=MESH)

    def send_rows(k, carry):
        dest = lax.rem(ep + k, n_ep)
        share_copy(dest, ep, dest).start()
        gather_copy(dest, ep, dest).start()
        return carry

    def await_rows(k, carry):
        source = lax.rem(ep + k, n_ep)
        share_copy(source, source, source).wait_recv()
        gather_copy(source, source, source).wait_recv()
        return carry

    lax.fori_loop(1, n_ep, send_rows, 0)
    lax.fori_loop(1, n_ep, await_rows, 0)

    everything = gathered[...].astype(F32).reshape(n_rows, width)
    mix_gate = jax.nn.sigmoid(jnp.sum(everything * mix[...].astype(F32), axis=1, keepdims=True))
    everything = everything.astype(BF16)

    members = n_ep * n_tp // EXPERTS
    expert = (ep * n_tp + tp) // members
    share_all = shares[...].reshape(n_rows, LANES).astype(BF16)
    one_hot = (lax.broadcasted_iota(jnp.int32, (8, LANES), 1) == expert).astype(F32).astype(BF16)
    share_row = dot(one_hot, share_all, ((1,), (1,)))
    present = (share_row > 0.0).astype(F32)
    row_j = lax.broadcasted_iota(jnp.int32, (n_rows, n_rows), 0)
    row_i = lax.broadcasted_iota(jnp.int32, (n_rows, n_rows), 1)
    shift = rows.bit_length() - 1
    same = ((row_j >> shift) == (row_i >> shift)) & (row_j <= row_i)
    rank = dot(present.astype(BF16), same.astype(F32).astype(BF16)) - 1.0
    n_slots = n_ep * cap
    slot = lax.broadcasted_iota(jnp.int32, (n_slots, n_rows), 0)
    block = lax.broadcasted_iota(jnp.int32, (n_slots, n_rows), 1) >> shift
    picked = ((slot - cap * block).astype(F32) == rank[0:1]) & (present[0:1] > 0.0)
    selector = picked.astype(F32)
    slot_share = jnp.sum(selector * share_row[0:1], axis=1, keepdims=True)
    selector = selector.astype(BF16)
    slots[0] = dot(selector, everything).astype(BF16)
    slot_copy = pltpu.make_async_remote_copy(
        slots.at[0], slots.at[1], slot_sem.at[0], slot_sem.at[1],
        device_id=(ep, other), device_id_type=MESH)
    slot_copy.start()

    l_dg.wait()
    l_du.wait()

    across = ((1,), (1,))
    up = dot(everything, du[...], across)
    d_hidden[...] = (jax.nn.silu(dot(everything, dg[...], across)) * up).astype(BF16)

    l_eg.wait()
    l_eu.wait()
    slot_copy.wait_recv()
    slot_rows = slots[...].reshape(2 * n_slots, width)

    def expert_up(cols):
        up = dot(slot_rows, eu[:, cols])
        e_hidden[:, cols] = (jax.nn.silu(dot(slot_rows, eg[:, cols])) * up).astype(BF16)

    tiled(e_hidden.shape[1], expert_up)
    l_ed.wait()

    chunks = scatter_out.shape[0]
    part = width // chunks

    def back_copy(c):
        return pltpu.make_async_remote_copy(
            theirs_out.at[c], theirs_in.at[c], back_sem.at[0, c], back_sem.at[1, c],
            device_id=(ep, other), device_id_type=MESH)

    def scatter_copy(c, dest, source):
        return pltpu.make_async_remote_copy(
            scatter_out.at[c, dest], scatter_in.at[c, source], r_send.at[c, dest], r_recv.at[c, source],
            device_id=(dest, tp), device_id_type=MESH)

    for c in range(chunks):
        value = dot(e_hidden[...], ed[:, c * part:(c + 1) * part])
        mine[c] = value[:n_slots]
        theirs_out[c] = value[n_slots:].astype(BF16)
        back_copy(c).start()
    l_dd.wait()

    for c in range(chunks):
        total = dot(d_hidden[...], dd[:, c * part:(c + 1) * part]) * mix_gate
        back_copy(c).wait_recv()
        result = ((mine[c] + theirs_in[c].astype(F32)) * slot_share).astype(BF16)
        total = total + dot(selector, result, ((0,), (0,)))
        scatter_out[c] = total.reshape(n_ep, rows, part).astype(BF16)

        def send_sums(k, carry):
            dest = lax.rem(ep + k, n_ep)
            scatter_copy(c, dest, ep).start()
            return carry

        lax.fori_loop(1, n_ep, send_sums, 0)

    for c in range(chunks):

        def add_sums(k, total):
            source = lax.rem(ep + n_ep - k, n_ep)
            scatter_copy(c, source, source).wait_recv()
            return total + scatter_in[c, source].astype(F32)

        begin = middle[:, c * part:(c + 1) * part] + scatter_out[c, ep].astype(F32)
        total = lax.fori_loop(1, n_ep, add_sums, begin)
        out[:, c * part:(c + 1) * part] = total.astype(BF16)

    pair_copy.wait_send()
    slot_copy.wait_send()
    for c in range(chunks):
        back_copy(c).wait_send()

    def finish(k, carry):
        dest = lax.rem(ep + k, n_ep)
        share_copy(dest, ep, dest).wait_send()
        gather_copy(dest, ep, dest).wait_send()
        for c in range(chunks):
            scatter_copy(c, dest, ep).wait_send()
        return carry

    lax.fori_loop(1, n_ep, finish, 0)


def shards(
    n_ep, n_tp,
    tokens, norm_attn, w_query, w_key, w_value, w_out, attn_bias, cache_keys, cache_values, lengths,
    norm_ffn, expert_gate, expert_up, expert_down, dense_gate_w, dense_up_w, dense_down_w, dense_mix,
    routes, route_weights,
):
    seqs, width = tokens.shape
    rows = seqs // n_tp
    heads = attn_bias.shape[0]
    cap = (rows * TOP + EXPERTS - 1) // EXPERTS + 1
    chunks = 4 if width % 512 == 0 else 1
    part = width // chunks
    weights = (w_query, w_key, w_value, w_out, cache_keys, cache_values, expert_gate, expert_up,
               expert_down, dense_gate_w.T, dense_up_w.T, dense_down_w)
    vmem = pl.BlockSpec(memory_space=pltpu.VMEM)
    smem = pl.BlockSpec(memory_space=pltpu.SMEM)
    hbm = pl.BlockSpec(memory_space=pl.ANY)
    n_slots = n_ep * cap
    ff, dense_ff = expert_gate.shape[1], dense_gate_w.shape[1]
    dma = pltpu.SemaphoreType.DMA
    scratch = [pltpu.VMEM(w.shape, w.dtype) for w in weights] + [
        pltpu.VMEM((seqs, heads, LANES), F32),
        pltpu.VMEM((seqs, heads, LANES), F32),
        pltpu.VMEM((seqs, heads * HEAD_DIM), BF16),
        pltpu.VMEM((n_tp, rows, width), F32),
        pltpu.VMEM((rows, width), F32),
        pltpu.VMEM((n_tp, rows, width), F32),
        pltpu.VMEM((rows, LANES), F32),
        pltpu.VMEM((n_ep, rows, width), BF16),
        pltpu.VMEM((n_ep, rows, LANES), F32),
        pltpu.VMEM((2, n_slots, width), BF16),
        pltpu.VMEM((2 * n_slots, ff), BF16),
        pltpu.VMEM((n_ep * rows, dense_ff), BF16),
        pltpu.VMEM((chunks, n_slots, part), F32),
        pltpu.VMEM((chunks, n_slots, part), BF16),
        pltpu.VMEM((chunks, n_slots, part), BF16),
        pltpu.VMEM((chunks, n_ep, rows, part), BF16),
        pltpu.VMEM((chunks, n_ep, rows, part), BF16),
        dma((10,)), dma((seqs,)), dma((seqs,)), dma((2,)),
        dma((n_ep,)), dma((n_ep,)), dma((n_ep,)), dma((n_ep,)),
        dma((2,)), dma((2, chunks)), dma((chunks, n_ep)), dma((chunks, n_ep)),
    ]
    results = pl.pallas_call(
        functools.partial(kernel, n_ep, n_tp),
        out_shape=(
            jax.ShapeDtypeStruct((rows, width), BF16),
            jax.ShapeDtypeStruct((seqs, w_key.shape[1]), BF16),
            jax.ShapeDtypeStruct((seqs, w_value.shape[1]), BF16),
        ),
        in_specs=[vmem, vmem, smem, smem, vmem, vmem, vmem, vmem] + [hbm] * 12,
        out_specs=(vmem, vmem, vmem),
        scratch_shapes=scratch,
        compiler_params=pltpu.CompilerParams(
            collective_id=0, has_side_effects=True, vmem_limit_bytes=67043328
        ),
    )(tokens, norm_attn[None], attn_bias, lengths, norm_ffn[None],
      dense_mix[None], routes.T, route_weights.T, *weights)
    return pl.pallas_call(
        hand_over,
        out_shape=tuple(jax.ShapeDtypeStruct(r.shape, r.dtype) for r in results),
        in_specs=[vmem] * 3,
        out_specs=(vmem, vmem, vmem),
    )(*results)


def hand_over(a, b, c, a_out, b_out, c_out):
    a_out[...] = a[...]
    b_out[...] = b[...]
    c_out[...] = c[...]


def solution(mesh):
    placed = (
        P("ep", None),
        P(),
        P(None, "tp"),
        P(None, "tp"),
        P(None, "tp"),
        P("tp", None),
        P("tp"),
        P("ep", None, "tp"),
        P("ep", None, "tp"),
        P("ep"),
        P(),
        P(None, ("ep", "tp")),
        P(None, ("ep", "tp")),
        P(("ep", "tp"), None),
        P(None, "ep"),
        P(None, "ep"),
        P("ep", None),
        P(),
        P(("ep", "tp"), None),
        P(("ep", "tp"), None),
    )
    return jax.shard_map(
        functools.partial(shards, mesh.shape["ep"], mesh.shape["tp"]),
        mesh=mesh,
        in_specs=placed,
        out_specs=(P(("ep", "tp"), None), P("ep", "tp"), P("ep", "tp")),
        check_vma=False,
    )
```
